32 devices in a mesh: ep: 8 (over z, x), tp: 4 (over y, core).
Axes of the slice: x: 2, y: 2, z: 4, core: 2. Of those that a mesh axis runs over, the one named last changes fastest.
Arguments:
- residual: bfloat16 [64, 2048], P(None, 'ep'), may hold values from -40 to 40
- norm_gain: float32 [2048], P('ep'), may hold values from 0.1 to 1.9
- query_weight: bfloat16 [2048, 2048], P('ep', 'tp'), may hold values from -0.125 to 0.125
- key_weight: bfloat16 [2048, 2048], P('ep', 'tp'), may hold values from -0.125 to 0.125
- value_weight: bfloat16 [2048, 4096], P('ep', 'tp'), may hold values from -0.125 to 0.125
- gate_weight: bfloat16 [2048, 4096], P('ep', 'tp'), may hold values from -0.125 to 0.125
- out_weight: bfloat16 [4096, 2048], P('tp', 'ep'), may hold values from -0.09375 to 0.09375
- prior_state: float32 [64, 16, 128, 256], P('ep', 'tp'), may hold values from -3 to 3
- lengths: int32 [64], P('ep'), may hold values from 1024 to 16383
- ffn_gain: float32 [2048], replicated, may hold values from 0.1 to 1.9
- expert_gate: bfloat16 [8, 2048, 2048], P('ep', None, 'tp'), may hold values from -0.5 to 0.5
- expert_up: bfloat16 [8, 2048, 2048], P('ep', None, 'tp'), may hold values from -0.5 to 0.5
- expert_down: bfloat16 [8, 2048, 2048], P('ep', 'tp'), may hold values from -0.03125 to 0.03125
- route_ids: int32 [64, 4], replicated, may hold values from 0 to 7, all different within a row; in each aligned block of 8 rows (0 to 7, 8 to 15, ...) at most 8 rows name the same one
- route_weight: float32 [64, 4], replicated, may hold values from 0.1 to 1
- dense_gate: bfloat16 [2048, 2048], P('ep', 'tp'), may hold values from -0.125 to 0.125
- dense_up: bfloat16 [2048, 2048], P('ep', 'tp'), may hold values from -0.125 to 0.125
- dense_down: bfloat16 [2048, 2048], P('tp', 'ep'), may hold values from -0.1875 to 0.1875
- mix_vector: bfloat16 [2048], P('ep'), may hold values from -0.125 to 0.125
Outputs:
- layer_out: bfloat16 [64, 2048], P(None, 'ep')
- new_state: float32 [64, 16, 128, 256], P('ep', 'tp')
The draws below stay inside these ranges and needn't reach their ends.
Inputs may be any that keep to these rules, and one draw needn't show every extreme that they name: `route_ids`: each row names 4 different experts; within each aligned block of 8 rows no expert is named by more than 8 rows, and in some block one expert is named by exactly 8 rows.
All inputs are finite; a program needn't handle non-finite values.
Results may differ from the reference program's by a relative error of at most 0.02.
Values may be sent and summed in bfloat16 or wider, within the bound.
A program may use at most 64 MiB of HBM per device.

```python
import math
import jax
import jax.numpy as jnp
import numpy as np
from jax import lax

D = 2048
HEADS = 16
KEY_DIM = 128
VAL_DIM = 256
FF = 2048
DENSE = 2048
TOPK = 4
B_DEV = 8
BATCH = 64
EXPERTS = 8
CAP = 8
SLOTS = 64
N_EP = 8
N_TP = 4


def draw_residual(key, part):
    base_key, row_key = jax.random.split(key, 2)
    columns = jnp.arange(D, dtype=jnp.float32) / (D - 1)
    column_scale = 0.35 * jnp.exp(jnp.log(8.0) * columns)
    row_draw = jax.random.uniform(row_key, (BATCH, 1), jnp.float32, 0.0, 1.0)
    row_scale = jnp.exp(jnp.log(10.0) * (row_draw - 0.5))
    base = jax.random.truncated_normal(base_key, -4.0, 4.0, (BATCH, D), jnp.float32)
    return (base * column_scale[None, :] * row_scale).astype(jnp.bfloat16)


def touch_ends(entries, own_key, smallest, largest):
    spot = [jax.random.randint(jax.random.fold_in(own_key, axis), (), 0, length) for axis, length in enumerate(entries.shape)]
    longest = entries.shape.index(max(entries.shape))
    next_to = spot[:longest] + [(spot[longest] + 1) % entries.shape[longest]] + spot[longest + 1:]
    return entries.at[tuple(spot)].set(smallest).at[tuple(next_to)].set(largest)


def with_spikes(array, stream_key, source, target, blocks, factor):
    owner, partner = [(jnp.arange(array.shape[dim]) // (array.shape[dim] // blocks)).reshape([-1 if axis == dim else 1 for axis in range(array.ndim)]) for dim in (source, target)]
    chosen = jax.random.permutation(stream_key, blocks)[partner]
    strong = (owner == chosen) | (owner == (partner + blocks // 2) % blocks)
    return jnp.where(strong, factor * array, array)


def steps_of(rng, shape, cuts, least, largest):
    def one(dim, parts):
        heights = jax.random.uniform(jax.random.fold_in(jax.random.fold_in(rng, 6), dim), (parts,), jnp.float32, least / len(cuts), largest / len(cuts))
        return jnp.repeat(jnp.exp(heights), shape[dim] // parts).reshape((-1,) + (1,) * (len(shape) - dim - 1))

    loudness = one(*cuts[0])
    for cut in cuts[1:]:
        loudness = loudness * one(*cut)
    return loudness


def deal_out(own_key, own, number, rows, amount, top, most, lean):
    ranking = jax.random.permutation(own_key, amount)
    crowded, ordinary = shares(amount, rows * top, most, lean, True), shares(amount, rows * top, most, lean, False)
    places = jnp.arange(amount)

    def named(sizes, turn):
        used = int((sizes > 0).sum())
        fixed = max(1, used // 4)
        passed = fixed + (places - fixed + turn * (used - fixed)) % max(1, amount - fixed)
        return jnp.zeros((amount,), jnp.int32).at[ranking[jnp.where(places < fixed, places, passed)]].set(jnp.asarray(sizes, jnp.int32))

    sizes = jnp.where(number % 4 == 0, named(crowded, number // 4), named(ordinary, number - number // 4 - 1))
    mixed = jax.random.permutation(jax.random.fold_in(own, 3), amount)
    source_of, receiver = mixed[0:amount // 2 * 2:2], mixed[1:amount // 2 * 2:2]
    room = jnp.minimum(sizes[source_of] - 1, most - sizes[receiver]) // 2
    room = jnp.where((source_of == ranking[0]) | (receiver == ranking[0]) | (sizes[receiver] == 0), 0, jnp.maximum(room, 0))
    passed = jax.random.randint(jax.random.fold_in(own, 4), (amount // 2,), 0, 1 << 20) % (room + 1)
    sizes = sizes.at[source_of].add(-passed).at[receiver].add(passed)
    members = jnp.searchsorted(jnp.cumsum(sizes), jnp.arange(rows * top), side="right").astype(jnp.int32)
    grid = members.reshape(top, rows).T
    grid = grid[jax.random.permutation(jax.random.fold_in(own, 1), rows)]
    turn = jax.random.randint(jax.random.fold_in(own, 2), (rows, 1), 0, top)
    return jnp.take_along_axis(grid, (jnp.arange(top)[None, :] + turn) % top, axis=1)


def shares(amount, total, most, lean, full):
    loads = [(1 << 20) // math.isqrt(rank ** lean) + 1 for rank in range(1, amount + 1)]
    largest = most if full else min(most, max(-(-total // amount), total * loads[0] // sum(loads)))
    least = 1 if total - largest >= amount - 1 else 0
    holding, rest = [largest] + [least] * (amount - 1), total - largest - least * (amount - 1)
    while rest > 0:
        movable = [i for i in range(1, amount) if holding[i] < largest] or [i for i in range(1, amount) if holding[i] < most]
        whole, left = sum([loads[i] for i in movable]), rest
        for i in movable:
            addition = min(most - holding[i], max(1, left * loads[i] // whole), rest)
            holding[i] = holding[i] + addition
            rest = rest - addition
    return np.array(holding)


def noise(own_key, extent, scale, reach, cuts=(), kind=jnp.bfloat16):
    values = scale * jax.random.normal(own_key, extent, jnp.float32)
    if cuts:
        values = values * steps_of(own_key, extent, cuts, -0.22, 0.18)
    return jnp.clip(values, -reach, reach).astype(kind)


def noise_with(own_key, dims, scale, most, shards, heavy, kind=jnp.bfloat16):
    entries = scale * jax.random.normal(own_key, dims, jnp.float32)
    if shards:
        entries = entries * steps_of(own_key, dims, shards, -0.22, 0.18)
    return jnp.clip(with_spikes(entries, jax.random.fold_in(own_key, 3), *heavy), -most, most).astype(kind)


def setup_inputs(seed: int = 0) -> dict:
    splits = jax.random.split(jax.random.key(seed), 20)
    residual = draw_residual(jax.random.fold_in(splits[19], 71), 0)
    norm_gain = jnp.clip(1.0 + 0.18 * jax.random.normal(splits[1], (D,), jnp.float32), 0.1, 1.9)
    query_weight = noise(splits[2], (D, HEADS * KEY_DIM), D ** -0.5, 0.125, ((0, 8), (1, 4)))
    key_weight = noise(splits[3], (D, HEADS * KEY_DIM), D ** -0.5, 0.125, ((0, 8), (1, 4)))
    value_weight = noise(splits[4], (D, HEADS * VAL_DIM), D ** -0.5, 0.125, ((0, 8), (1, 4)))
    gate_weight = noise(splits[5], (D, HEADS * VAL_DIM), D ** -0.5, 0.125, ((0, 8), (1, 4)))
    out_weight = noise(splits[6], (HEADS * VAL_DIM, D), (HEADS * VAL_DIM) ** -0.5, 0.09375, ((0, 4), (1, 8)))
    prior_state = noise(splits[7], (BATCH, HEADS, KEY_DIM, VAL_DIM), 0.5, 3.0, ((0, 8), (1, 4)), jnp.float32)
    lengths = touch_ends(jax.random.randint(splits[8], (BATCH,), 1024, 16384), jax.random.fold_in(splits[8], 1), 1024, 16383).astype(jnp.int32)
    ffn_gain = jnp.clip(1.0 + 0.18 * jax.random.normal(splits[9], (D,), jnp.float32), 0.1, 1.9)
    expert_gate = noise(splits[10], (EXPERTS, D, FF), (D // 16) ** -0.5, 0.5, ((0, 8), (2, 4)))
    expert_up = noise(splits[11], (EXPERTS, D, FF), (D // 16) ** -0.5, 0.5, ((0, 8), (2, 4)))
    expert_down = noise(splits[12], (EXPERTS, FF, D), (FF * 16) ** -0.5, 0.03125, ((0, 8), (1, 4)))
    route_ids_keys = jax.random.split(jax.random.fold_in(splits[13], 1), BATCH // B_DEV)
    route_ids_turns = jax.random.permutation(jax.random.fold_in(splits[13], 3), BATCH // B_DEV)
    route_ids = jax.vmap(lambda own, number: deal_out(jax.random.fold_in(splits[13], 2), own, number, B_DEV, EXPERTS, TOPK, CAP, 2))(route_ids_keys, route_ids_turns).reshape((BATCH, TOPK))
    route_weight = jnp.clip(jnp.exp(jax.random.uniform(splits[14], (BATCH, TOPK), jnp.float32, math.log(0.1), math.log(1.0))), 0.1, 1.0)
    dense_gate = noise(splits[15], (D, DENSE), D ** -0.5, 0.125, ((0, 8), (1, 4)))
    dense_up = noise(splits[16], (D, DENSE), D ** -0.5, 0.125, ((0, 8), (1, 4)))
    dense_down = noise_with(splits[17], (DENSE, D), DENSE ** -0.5, 0.1875, ((0, 4), (1, 8)), (0, 1, 8, 2.0))
    mix_vector = noise(splits[18], (D,), D ** -0.5, 0.125, ((0, 8),))
    return {"residual": residual, "norm_gain": norm_gain, "query_weight": query_weight, "key_weight": key_weight, "value_weight": value_weight, "gate_weight": gate_weight, "out_weight": out_weight, "prior_state": prior_state, "lengths": lengths, "ffn_gain": ffn_gain, "expert_gate": expert_gate, "expert_up": expert_up, "expert_down": expert_down, "route_ids": route_ids, "route_weight": route_weight, "dense_gate": dense_gate, "dense_up": dense_up, "dense_down": dense_down, "mix_vector": mix_vector}


norm_eps = 1e-06
clamp_limit = 7.0
gate_alpha = 1.702

def rotate_half(vectors, positions):
    half_dim = vectors.shape[-1] // 2
    inverse = 1.0 / 10000.0 ** jnp.linspace(0.0, 1.0, half_dim, dtype=jnp.float32)
    angles = positions.astype(jnp.float32)[:, None] * inverse[None, :]
    cosine = jnp.cos(angles)[:, None, :]
    sine_part = jnp.sin(angles)[:, None, :]
    first_half = vectors[..., :half_dim]
    second_half = vectors[..., half_dim:]
    return jnp.concatenate([first_half * cosine - second_half * sine_part, second_half * cosine + first_half * sine_part], axis=-1)

def grouped_product(left_rows, right_rows, groups):
    block_width = left_rows.shape[1] // groups
    left_blocks = left_rows.reshape(left_rows.shape[0], groups, block_width).astype(jnp.float32)
    right_blocks = right_rows.reshape(groups, block_width, right_rows.shape[1]).astype(jnp.float32)
    partial_value = jnp.einsum('bgw,gwd->gbd', left_blocks, right_blocks)
    rounded = lax.optimization_barrier(partial_value.astype(jnp.bfloat16))
    return lax.optimization_barrier(jnp.sum(rounded.astype(jnp.float32), axis=0))

def slot_index(route_ids, groups, capacity, experts):
    pair_ids = route_ids.reshape(groups, -1)
    labels = jnp.arange(experts, dtype=jnp.int32)
    onehot = (pair_ids[:, :, None] == labels[None, None, :]).astype(jnp.int32)
    earlier = jnp.cumsum(onehot, axis=1) - onehot
    within = lax.optimization_barrier(jnp.sum(earlier * onehot, axis=2))
    offset = jnp.arange(groups, dtype=jnp.int32)[:, None] * capacity
    return (pair_ids * (groups * capacity) + offset + within).reshape(-1).astype(jnp.int32)

def source_rows(target, total_rows, topk_count, table_size):
    owners = jnp.arange(target.shape[0], dtype=jnp.int32) // topk_count
    return jnp.full((table_size,), total_rows, jnp.int32).at[target].set(owners)

def expert_block(rows_in, gain, gate_w, up_w, down_w, groups):
    rows_float = rows_in.astype(jnp.float32)
    row_norm = lax.rsqrt(lax.optimization_barrier(jnp.mean(rows_float * rows_float, axis=1, keepdims=True)) + norm_eps)
    normed = (rows_float * gain).astype(jnp.bfloat16)
    gate_val = jnp.minimum(jnp.dot(normed, gate_w, preferred_element_type=jnp.float32) * row_norm, clamp_limit)
    up_val = jnp.clip(jnp.dot(normed, up_w, preferred_element_type=jnp.float32) * row_norm, -clamp_limit, clamp_limit)
    hidden = ((up_val + 1.0) * gate_val * jax.nn.sigmoid(gate_alpha * gate_val)).astype(jnp.bfloat16)
    return grouped_product(hidden, down_w, groups).astype(jnp.bfloat16)

def reference(residual, norm_gain, query_weight, key_weight, value_weight, gate_weight, out_weight, prior_state, lengths, ffn_gain, expert_gate, expert_up, expert_down, route_ids, route_weight, dense_gate, dense_up, dense_down, mix_vector):
    batch_rows = residual.shape[0]
    residual_float = residual.astype(jnp.float32)
    row_scale = lax.rsqrt(lax.optimization_barrier(jnp.mean(residual_float * residual_float, axis=1, keepdims=True)) + norm_eps)
    normed_in = (residual_float * norm_gain).astype(jnp.bfloat16)
    query = jnp.dot(normed_in, query_weight, preferred_element_type=jnp.float32) * row_scale
    key_raw = jnp.dot(normed_in, key_weight, preferred_element_type=jnp.float32) * row_scale
    value_proj = jnp.dot(normed_in, value_weight, preferred_element_type=jnp.float32) * row_scale
    gate_pre = jnp.dot(normed_in, gate_weight, preferred_element_type=jnp.float32) * row_scale
    query_rot = rotate_half(query.reshape(batch_rows, HEADS, KEY_DIM), lengths)
    key_rot = rotate_half(key_raw.reshape(batch_rows, HEADS, KEY_DIM), lengths) * KEY_DIM ** (-0.5)
    values = value_proj.reshape(batch_rows, HEADS, VAL_DIM)
    decay_rate = 1.0 - jnp.exp2(-1.0 - 0.5 * jnp.arange(HEADS, dtype=jnp.float32))
    new_state = decay_rate[None, :, None, None] * prior_state + key_rot[:, :, :, None] * values[:, :, None, :]
    state_read = jnp.einsum('bhk,bhkv->bhv', query_rot, new_state, precision=lax.Precision.HIGHEST)
    normed = state_read * lax.rsqrt(lax.optimization_barrier(jnp.mean(state_read * state_read, axis=-1, keepdims=True)) + norm_eps)
    gated_out = (normed * jax.nn.silu(gate_pre.reshape(batch_rows, HEADS, VAL_DIM))).astype(jnp.bfloat16)
    gated_out = gated_out.reshape(batch_rows, HEADS * VAL_DIM)
    attn_out = grouped_product(gated_out, out_weight, N_TP)
    after_mixer = (residual_float + attn_out).astype(jnp.bfloat16)
    target = slot_index(route_ids, N_EP, CAP, EXPERTS)
    slot_source = source_rows(target, batch_rows, TOPK, EXPERTS * SLOTS)
    padded = jnp.concatenate([after_mixer, jnp.zeros((1, D), jnp.bfloat16)], axis=0)
    expert_in = padded[slot_source].reshape(EXPERTS, SLOTS, D)

    def run_expert(operands):
        rows_in, gate_w, up_w, down_w = operands
        return expert_block(rows_in, ffn_gain, gate_w, up_w, down_w, N_TP)
    expert_out = lax.map(run_expert, (expert_in, expert_gate, expert_up, expert_down))
    picked = expert_out.reshape(EXPERTS * SLOTS, D)[target].reshape(batch_rows, TOPK, D).astype(jnp.float32)
    routed = lax.optimization_barrier(jnp.sum(picked * route_weight[:, :, None], axis=1))
    after_float = after_mixer.astype(jnp.float32)
    ffn_scale = lax.rsqrt(lax.optimization_barrier(jnp.mean(after_float * after_float, axis=1, keepdims=True)) + norm_eps)
    normed_ffn = (after_float * ffn_gain).astype(jnp.bfloat16)
    dense_g = jnp.dot(normed_ffn, dense_gate, preferred_element_type=jnp.float32) * ffn_scale
    dense_u = jnp.dot(normed_ffn, dense_up, preferred_element_type=jnp.float32) * ffn_scale
    dense_act = (jax.nn.silu(dense_g) * dense_u).astype(jnp.bfloat16)
    dense_out = grouped_product(dense_act, dense_down, N_TP)
    mix_logit = jnp.dot(normed_ffn, mix_vector, preferred_element_type=jnp.float32)
    dense_mix = jax.nn.sigmoid(ffn_scale[:, 0] * mix_logit)
    layer_out = (after_float + routed + dense_mix[:, None] * dense_out).astype(jnp.bfloat16)
    return (layer_out, new_state)
```

```python
import jax
import jax.numpy as jnp
from jax import lax
from jax.experimental import pallas as pl
from jax.experimental.pallas import tpu as pltpu
from jax.sharding import PartitionSpec as P

D = 2048
KEY_DIM = 128
VAL_DIM = 256


norm_eps = 1e-06
clamp_limit = 7.0
gate_alpha = 1.702


def rotate_half(vectors, positions):
    half_dim = vectors.shape[-1] // 2
    inverse = 1.0 / 10000.0 ** jnp.linspace(0.0, 1.0, half_dim, dtype=jnp.float32)
    angles = positions.astype(jnp.float32)[:, None] * inverse[None, :]
    cosine = jnp.cos(angles)[:, None, :]
    sine_part = jnp.sin(angles)[:, None, :]
    first_half = vectors[..., :half_dim]
    second_half = vectors[..., half_dim:]
    return jnp.concatenate(
        [
            first_half * cosine - second_half * sine_part,
            second_half * cosine + first_half * sine_part,
        ],
        axis=-1,
    )


def slot_index(route_ids, groups, capacity, experts):
    pair_ids = route_ids.reshape(groups, -1)
    labels = jnp.arange(experts, dtype=jnp.int32)
    onehot = (pair_ids[:, :, None] == labels[None, None, :]).astype(jnp.int32)
    earlier = jnp.cumsum(onehot, axis=1) - onehot
    within = jnp.sum(earlier * onehot, axis=2)
    offset = jnp.arange(groups, dtype=jnp.int32)[:, None] * capacity
    return (pair_ids * (groups * capacity) + offset + within).reshape(-1)


def source_rows(target, total_rows, topk_count, table_size):
    owners = jnp.arange(target.shape[0], dtype=jnp.int32) // topk_count
    return jnp.full((table_size,), total_rows, jnp.int32).at[target].set(owners)


def rounded_product(left_rows, right_rows):
    partial_value = jnp.dot(left_rows, right_rows, preferred_element_type=jnp.float32)
    return lax.optimization_barrier(partial_value.astype(jnp.bfloat16))


def per_device(
    residual,
    norm_gain,
    query_weight,
    key_weight,
    value_weight,
    gate_weight,
    out_weight,
    prior_state,
    lengths,
    ffn_gain,
    expert_gate,
    expert_up,
    expert_down,
    route_ids,
    route_weight,
    dense_gate,
    dense_up,
    dense_down,
    mix_vector,
):
    ep_count = lax.axis_size("ep")
    ep_index = lax.axis_index("ep")
    batch_rows, local_width = residual.shape
    own_rows = batch_rows // ep_count
    topk_count = route_ids.shape[1]
    residual_float = residual.astype(jnp.float32)
    squares = jnp.sum(residual_float * residual_float, axis=1)
    normed_in = (residual_float * norm_gain).astype(jnp.bfloat16)
    all_weights = jnp.concatenate([query_weight, key_weight, value_weight, gate_weight], axis=1)
    whole_terms = jnp.dot(normed_in, all_weights, preferred_element_type=jnp.float32)
    projected, own_squares = (
        lax.psum_scatter(whole_terms, "ep", scatter_dimension=0, tiled=True),
        lax.psum_scatter(squares, "ep", scatter_dimension=0, tiled=True),
    )
    row_scale = lax.rsqrt(own_squares / D + norm_eps)[:, None]
    key_cols = query_weight.shape[1]
    value_cols = value_weight.shape[1]
    heads_here = key_cols // KEY_DIM
    projected = projected * row_scale
    query_rot = rotate_half(projected[:, :key_cols].reshape(own_rows, heads_here, KEY_DIM), lengths)
    key_rot = rotate_half(
        projected[:, key_cols : 2 * key_cols].reshape(own_rows, heads_here, KEY_DIM), lengths
    ) * KEY_DIM ** (-0.5)
    values = projected[:, 2 * key_cols : 2 * key_cols + value_cols].reshape(
        own_rows, heads_here, VAL_DIM
    )
    gate_pre = projected[:, 2 * key_cols + value_cols :].reshape(own_rows, heads_here, VAL_DIM)
    head_ids = lax.axis_index("tp") * heads_here + jnp.arange(heads_here, dtype=jnp.int32)
    decay_rate = 1.0 - jnp.exp2(-1.0 - 0.5 * head_ids.astype(jnp.float32))
    new_state = (
        decay_rate[None, :, None, None] * prior_state
        + key_rot[:, :, :, None] * values[:, :, None, :]
    )
    state_read = jnp.einsum("bhk,bhkv->bhv", query_rot, new_state, precision=lax.Precision.HIGHEST)
    normed = state_read * lax.rsqrt(
        jnp.mean(state_read * state_read, axis=-1, keepdims=True) + norm_eps
    )
    gated_out = (
        (normed * jax.nn.silu(gate_pre))
        .astype(jnp.bfloat16)
        .reshape(own_rows, heads_here * VAL_DIM)
    )
    head_terms = rounded_product(lax.all_gather(gated_out, "ep", axis=0, tiled=True), out_weight)
    attn_out = lax.psum(head_terms.astype(jnp.float32).astype(jnp.bfloat16), "tp").astype(
        jnp.float32
    )
    after_mixer = (residual_float + attn_out).astype(jnp.bfloat16)
    capacity = max(2, 2 * own_rows * topk_count // ep_count)
    slot_count = ep_count * capacity
    target = slot_index(route_ids, ep_count, capacity, ep_count)
    slot_source = source_rows(target, batch_rows, topk_count, ep_count * slot_count)
    padded = jnp.concatenate([after_mixer, jnp.zeros((1, local_width), jnp.bfloat16)], axis=0)
    outgoing = padded[slot_source].reshape(ep_count, slot_count, local_width)
    arrived = lax.all_to_all(outgoing, "ep", split_axis=0, concat_axis=2, tiled=True)[0]
    rows_float = arrived.astype(jnp.float32)
    row_norm = lax.rsqrt(jnp.mean(rows_float * rows_float, axis=1, keepdims=True) + norm_eps)
    normed_rows = (rows_float * ffn_gain).astype(jnp.bfloat16)
    gate_val = jnp.minimum(
        jnp.dot(normed_rows, expert_gate[0], preferred_element_type=jnp.float32) * row_norm,
        clamp_limit,
    )
    up_val = jnp.clip(
        jnp.dot(normed_rows, expert_up[0], preferred_element_type=jnp.float32) * row_norm,
        -clamp_limit,
        clamp_limit,
    )
    hidden = ((up_val + 1.0) * gate_val * jax.nn.sigmoid(gate_alpha * gate_val)).astype(
        jnp.bfloat16
    )
    expert_part = rounded_product(hidden, expert_down[0]).astype(jnp.float32)
    expert_sum = lax.psum(expert_part.astype(jnp.bfloat16), "tp")
    returned = lax.all_to_all(expert_sum[None], "ep", split_axis=2, concat_axis=0, tiled=True)
    picked = returned.reshape(ep_count * slot_count, local_width)[target]
    picked = picked.reshape(batch_rows, topk_count, local_width).astype(jnp.float32)
    routed = jnp.sum(picked * route_weight[:, :, None], axis=1)
    after_float = after_mixer.astype(jnp.float32)
    gain_here = lax.dynamic_slice_in_dim(ffn_gain, ep_index * local_width, local_width, 0)
    normed_ffn = (after_float * gain_here).astype(jnp.bfloat16)
    dense_cols = dense_gate.shape[1]
    both_terms = jnp.dot(
        normed_ffn,
        jnp.concatenate([dense_gate, dense_up], axis=1),
        preferred_element_type=jnp.float32,
    )
    mix_term = jnp.dot(normed_ffn, mix_vector, preferred_element_type=jnp.float32)
    both_terms, ffn_squares, mix_logit = lax.psum(
        (both_terms, jnp.sum(after_float * after_float, axis=1), mix_term), "ep"
    )
    ffn_scale = lax.rsqrt(ffn_squares / D + norm_eps)[:, None]
    dense_act = (
        jax.nn.silu(both_terms[:, :dense_cols] * ffn_scale)
        * (both_terms[:, dense_cols:] * ffn_scale)
    ).astype(jnp.bfloat16)
    dense_part = rounded_product(dense_act, dense_down).astype(jnp.float32)
    dense_out = lax.psum(dense_part.astype(jnp.bfloat16), "tp").astype(jnp.float32)
    dense_mix = jax.nn.sigmoid(ffn_scale[:, 0] * mix_logit)
    layer_out = (after_float + routed + dense_mix[:, None] * dense_out).astype(jnp.bfloat16)
    return (layer_out, new_state)


F32 = jnp.float32
BF16 = jnp.bfloat16
MESH = pl.DeviceIdType.MESH
PROJ, SQUARE, MIX, HEAD, ROWS, DENSE_SUM, DENSE_ACT, BACK = range(8)
ATTN, FINAL = range(2)


def fused_kernel(
    residual, norm_gain, cosine, sine, gains, route_ids, route_weight, mix_own,
    query_hbm, key_hbm, value_hbm, gate_hbm, out_hbm, prior_hbm,
    egate_hbm, eup_hbm, edown_hbm, dgate_hbm, dup_hbm, ddown_hbm,
    layer_out, key_out, value_out,
    query_w, key_w, value_w, gate_w, out_w, prior, prior_half,
    egate, eup, edown, dgate, dup, ddown,
    proj_send, proj_recv, sq_send, sq_recv, mix_all, heads_all, attn_all,
    rows_all, square_rows, dense_send, dense_recv, act_all, back_send, back_recv, final_all,
    load_sem, send_sem, recv_sem, tp_send, tp_recv,
):
    ep, batch, width = rows_all.shape
    tp = attn_all.shape[0]
    own = batch // ep
    full = ep * width
    me = lax.axis_index("ep")
    lane = lax.axis_index("tp")
    pairs = [
        (query_hbm, query_w), (key_hbm, key_w), (value_hbm, value_w), (gate_hbm, gate_w),
        (prior_hbm, prior), (out_hbm, out_w), (dgate_hbm, dgate), (dup_hbm, dup),
        (egate_hbm, egate), (eup_hbm, eup), (edown_hbm, edown), (ddown_hbm, ddown),
    ]
    loads = [pltpu.make_async_copy(a, b, load_sem.at[i]) for i, (a, b) in enumerate(pairs)]
    barrier = pltpu.get_barrier_semaphore()
    for d in range(1, ep):
        pl.semaphore_signal(
            barrier, inc=1, device_id=(lax.rem(me + d, ep), lane), device_id_type=MESH
        )
    for d in range(1, tp):
        pl.semaphore_signal(
            barrier, inc=1, device_id=(me, lax.rem(lane + d, tp)), device_id_type=MESH
        )
    for load in loads:
        load.start()

    def to_ep(phase, d, source, target):
        return pltpu.make_async_remote_copy(
            src_ref=source,
            dst_ref=target,
            send_sem=send_sem.at[phase, d],
            recv_sem=recv_sem.at[phase, d],
            device_id=(lax.rem(me + d, ep), lane),
            device_id_type=MESH,
        )

    def to_tp(phase, d, source, target):
        return pltpu.make_async_remote_copy(
            src_ref=source,
            dst_ref=target,
            send_sem=tp_send.at[phase, d],
            recv_sem=tp_recv.at[phase, d],
            device_id=(me, lax.rem(lane + d, tp)),
            device_id_type=MESH,
        )

    sent = []

    def go(copy):
        copy.start()
        sent.append(copy)

    def peer(d):
        return lax.rem(me + d, ep)

    def sender(d):
        return lax.rem(me + ep - d, ep)

    def got(phase, d, buffer):
        to_ep(phase, d, buffer, buffer).wait_recv()

    resid = residual[...].astype(F32)
    squares = jnp.sum(resid * resid, axis=1, keepdims=True)
    squares = jnp.broadcast_to(squares, (batch, sq_send.shape[2]))
    for e in range(ep):
        sq_send[e] = squares[e * own : (e + 1) * own]
    normed_in = (resid * norm_gain[...]).astype(BF16)
    offset = 0
    for load, weight in zip(loads[:4], (query_w, key_w, value_w, gate_w)):
        load.wait()
        cols = weight.shape[1]
        step = min(cols, 512)
        for c in range(0, cols, step):
            terms = jnp.dot(normed_in, weight[:, c : c + step], preferred_element_type=F32)
            for e in range(ep):
                proj_send[e, :, offset + c : offset + c + step] = terms[
                    e * own : (e + 1) * own
                ].astype(BF16)
        offset += cols
    mix_all[me] = mix_own[...]
    pl.semaphore_wait(barrier, ep + tp - 2)
    for d in range(1, ep):
        go(to_ep(SQUARE, d, sq_send.at[peer(d)], sq_recv.at[d]))
        go(to_ep(PROJ, d, proj_send.at[peer(d)], proj_recv.at[d]))
    for d in range(1, ep):
        go(to_ep(MIX, d, mix_own, mix_all.at[me]))
    heads = prior.shape[1]
    loads[4].wait()
    for b in range(own):
        for h in range(heads):
            prior_half[b, h] = prior[b, h].astype(BF16)
    route_col = jnp.sum(
        jnp.where(route_ids[...] == me, route_weight[...], 0.0), axis=1, keepdims=True
    )
    total_sq = sq_send[me]
    projected = proj_send[me].astype(F32)
    for d in range(1, ep):
        got(SQUARE, d, sq_recv.at[d])
        total_sq = total_sq + sq_recv[d]
        got(PROJ, d, proj_recv.at[d])
        projected = projected + proj_recv[d].astype(F32)
    projected = projected * lax.rsqrt(total_sq / full + norm_eps)[:, :1]
    key_cols = query_w.shape[1]
    value_cols = value_w.shape[1]
    value_out[...] = projected[:, 2 * key_cols : 2 * key_cols + value_cols]
    row_ids = lax.broadcasted_iota(jnp.int32, (own, VAL_DIM), 0)
    for h in range(heads):
        ks = slice(h * KEY_DIM, (h + 1) * KEY_DIM)
        q = projected[:, ks]
        k = projected[:, key_cols + h * KEY_DIM : key_cols + (h + 1) * KEY_DIM]
        q = q * cosine[...] + pltpu.roll(q, KEY_DIM // 2, 1) * sine[...]
        k = (k * cosine[...] + pltpu.roll(k, KEY_DIM // 2, 1) * sine[...]) * KEY_DIM ** (-0.5)
        key_out[:, ks] = k
        start = 2 * key_cols + h * VAL_DIM
        v = projected[:, start : start + VAL_DIM]
        gate_pre = projected[:, start + value_cols : start + value_cols + VAL_DIM]
        q_half = q.astype(BF16)
        past = jnp.zeros((own, VAL_DIM), F32)
        for b in range(own):
            every = jnp.dot(q_half, prior_half[b, h], preferred_element_type=F32)
            past = past + jnp.where(row_ids == b, every, 0.0)
        head_id = jnp.full((own, VAL_DIM), lane * heads + h, jnp.int32).astype(F32)
        decay = 1.0 - jnp.exp((head_id * 0.5 + 1.0) * -0.6931471805599453)
        read = decay * past + jnp.sum(q * k, axis=1, keepdims=True) * v
        normed = read * lax.rsqrt(jnp.mean(read * read, axis=1, keepdims=True) + norm_eps)
        heads_all[me, :, h * VAL_DIM : (h + 1) * VAL_DIM] = (
            normed * (gate_pre / (1.0 + jnp.exp(-gate_pre)))
        ).astype(BF16)

    for d in range(1, ep):
        go(to_ep(HEAD, d, heads_all.at[me], heads_all.at[me]))
    loads[5].wait()
    for d in range(1, ep):
        got(HEAD, d, heads_all.at[sender(d)])
    gated = jnp.concatenate([heads_all[e].astype(F32) for e in range(ep)], axis=0)
    attn_all[lane] = jnp.dot(
        gated.astype(BF16), out_w[...], preferred_element_type=F32
    ).astype(BF16)
    for d in range(1, tp):
        go(to_tp(ATTN, d, attn_all.at[lane], attn_all.at[lane]))
    for d in range(1, tp):
        slot = attn_all.at[lax.rem(lane + tp - d, tp)]
        to_tp(ATTN, d, slot, slot).wait_recv()
    attn = attn_all[0].astype(F32)
    for t in range(1, tp):
        attn = attn + attn_all[t].astype(F32)
    after = (resid + attn).astype(BF16)
    rows_all[me] = after
    for d in range(1, ep):
        go(to_ep(ROWS, d, rows_all.at[me], rows_all.at[me]))

    after_float = after.astype(F32)
    own_normed = (after_float * gains[me]).astype(BF16)
    dense_cols = dgate.shape[1]
    for i, weight in enumerate((dgate, dup)):
        loads[6 + i].wait()
        terms = jnp.dot(own_normed, weight[...], preferred_element_type=F32)
        for e in range(ep):
            dense_send[e, :, i * dense_cols : (i + 1) * dense_cols] = terms[
                e * own : (e + 1) * own
            ].astype(BF16)
    for d in range(1, ep):
        go(to_ep(DENSE_SUM, d, dense_send.at[peer(d)], dense_recv.at[d]))

    loads[8].wait()
    loads[9].wait()
    gate_acc = up_acc = None
    sq_acc = logit = None
    for d in range(ep):
        e = sender(d)
        if d:
            got(ROWS, d, rows_all.at[e])
            got(MIX, d, mix_all.at[e])
        z = rows_all[e].astype(F32)
        zn = (z * gains[e]).astype(BF16)
        depth = pl.ds(pl.multiple_of(e * width, width), width)
        g = jnp.dot(zn, egate[0, depth, :], preferred_element_type=F32)
        u = jnp.dot(zn, eup[0, depth, :], preferred_element_type=F32)
        s = jnp.sum(z * z, axis=1, keepdims=True)
        m = jnp.sum(zn.astype(F32) * mix_all[e], axis=1, keepdims=True)
        if d:
            gate_acc, up_acc, sq_acc, logit = gate_acc + g, up_acc + u, sq_acc + s, logit + m
        else:
            gate_acc, up_acc, sq_acc, logit = g, u, s, m
    scale = lax.rsqrt(sq_acc / full + norm_eps)
    square_rows[...] = jnp.broadcast_to(scale, square_rows.shape)
    both = dense_send[me].astype(F32)
    for d in range(1, ep):
        got(DENSE_SUM, d, dense_recv.at[d])
        both = both + dense_recv[d].astype(F32)
    both = both * square_rows[pl.ds(pl.multiple_of(me * own, own), own), :][:, :1]
    dg = both[:, :dense_cols]
    act_all[me] = (dg / (1.0 + jnp.exp(-dg)) * both[:, dense_cols:]).astype(BF16)
    for d in range(1, ep):
        go(to_ep(DENSE_ACT, d, act_all.at[me], act_all.at[me]))
    gate_val = jnp.minimum(gate_acc * scale, clamp_limit)
    up_val = jnp.clip(up_acc * scale, -clamp_limit, clamp_limit)
    hidden = ((up_val + 1.0) * gate_val / (1.0 + jnp.exp(-gate_alpha * gate_val))).astype(BF16)
    loads[10].wait()
    for d in list(range(1, ep)) + [0]:
        e = peer(d)
        columns = pl.ds(pl.multiple_of(e * width, width), width)
        part = jnp.dot(hidden, edown[0, :, columns], preferred_element_type=F32) * route_col
        if d:
            back_send[d] = part.astype(BF16)
            go(to_ep(BACK, d, back_send.at[d], back_recv.at[d]))
    mixed = part
    loads[11].wait()
    for d in range(1, ep):
        got(DENSE_ACT, d, act_all.at[sender(d)])
    act = jnp.concatenate([act_all[e].astype(F32) for e in range(ep)], axis=0)
    dense_part = jnp.dot(act.astype(BF16), ddown[...], preferred_element_type=F32)
    mixed = mixed + dense_part / (1.0 + jnp.exp(-(scale * logit)))
    for d in range(1, ep):
        got(BACK, d, back_recv.at[d])
        mixed = mixed + back_recv[d].astype(F32)
    final_all[lane] = mixed.astype(BF16)
    for d in range(1, tp):
        go(to_tp(FINAL, d, final_all.at[lane], final_all.at[lane]))
    for d in range(1, tp):
        slot = final_all.at[lax.rem(lane + tp - d, tp)]
        to_tp(FINAL, d, slot, slot).wait_recv()
    result = after_float
    for t in range(tp):
        result = result + final_all[t].astype(F32)
    layer_out[...] = result.astype(BF16)
    for copy in sent:
        copy.wait_send()


def fused_device(
    residual, norm_gain, query_weight, key_weight, value_weight, gate_weight, out_weight,
    prior_state, lengths, ffn_gain, expert_gate, expert_up, expert_down, route_ids,
    route_weight, dense_gate, dense_up, dense_down, mix_vector,
):
    ep, tp = lax.axis_size("ep"), lax.axis_size("tp")
    batch, width = residual.shape
    own, heads = prior_state.shape[:2]
    half = KEY_DIM // 2
    inverse = 1.0 / 10000.0 ** jnp.linspace(0.0, 1.0, half, dtype=F32)
    angles = lengths.astype(F32)[:, None] * inverse[None, :]
    cosine, sine = jnp.cos(angles), jnp.sin(angles)
    cosine = jnp.concatenate([cosine, cosine], axis=1)
    sine = jnp.concatenate([-sine, sine], axis=1)
    key_cols, value_cols = query_weight.shape[1], value_weight.shape[1]
    all_cols = 2 * key_cols + 2 * value_cols
    dense_cols = dense_gate.shape[1]
    large = (
        query_weight, key_weight, value_weight, gate_weight, out_weight, prior_state,
        expert_gate, expert_up, expert_down, dense_gate, dense_up, dense_down,
    )
    held = [pltpu.VMEM(a.shape, a.dtype) for a in large]
    held.insert(6, pltpu.VMEM(prior_state.shape, BF16))
    vmem = pl.BlockSpec(memory_space=pltpu.VMEM)
    scratch = held + [
        pltpu.VMEM((ep, own, all_cols), BF16),
        pltpu.VMEM((ep, own, all_cols), BF16),
        pltpu.VMEM((ep, own, 128), F32),
        pltpu.VMEM((ep, own, 128), F32),
        pltpu.VMEM((ep, 1, width), F32),
        pltpu.VMEM((ep, own, value_cols), BF16),
        pltpu.VMEM((tp, batch, width), BF16),
        pltpu.VMEM((ep, batch, width), BF16),
        pltpu.VMEM((batch, 128), F32),
        pltpu.VMEM((ep, own, 2 * dense_cols), BF16),
        pltpu.VMEM((ep, own, 2 * dense_cols), BF16),
        pltpu.VMEM((ep, own, dense_cols), BF16),
        pltpu.VMEM((ep, batch, width), BF16),
        pltpu.VMEM((ep, batch, width), BF16),
        pltpu.VMEM((tp, batch, width), BF16),
        pltpu.SemaphoreType.DMA((12,)),
        pltpu.SemaphoreType.DMA((8, ep)),
        pltpu.SemaphoreType.DMA((8, ep)),
        pltpu.SemaphoreType.DMA((2, tp)),
        pltpu.SemaphoreType.DMA((2, tp)),
    ]
    layer_out, key_rot, values = pl.pallas_call(
        fused_kernel,
        out_shape=(
            jax.ShapeDtypeStruct((batch, width), BF16),
            jax.ShapeDtypeStruct((own, key_cols), F32),
            jax.ShapeDtypeStruct((own, value_cols), F32),
        ),
        in_specs=[vmem] * 8 + [pl.BlockSpec(memory_space=pl.ANY)] * 12,
        out_specs=(vmem, vmem, vmem),
        scratch_shapes=scratch,
        compiler_params=pltpu.CompilerParams(
            collective_id=0, has_side_effects=True, vmem_limit_bytes=56 * 1024 * 1024
        ),
    )(
        residual, norm_gain[None, :], cosine, sine, ffn_gain.reshape(ep, 1, width),
        route_ids, route_weight, mix_vector.astype(F32)[None, :], *large,
    )
    head_ids = lax.axis_index("tp") * heads + jnp.arange(heads, dtype=jnp.int32)
    decay_rate = 1.0 - jnp.exp2(-1.0 - 0.5 * head_ids.astype(F32))
    key_rot = key_rot.reshape(own, heads, KEY_DIM)
    values = values.reshape(own, heads, VAL_DIM)
    new_state = (
        decay_rate[None, :, None, None] * prior_state
        + key_rot[:, :, :, None] * values[:, :, None, :]
    )
    return (layer_out, new_state)


def any_device(*arrays):
    residual, prior_state, dense_gate = arrays[0], arrays[7], arrays[15]
    own = prior_state.shape[0]
    aligned = residual.shape[1] % 128 == 0 and dense_gate.shape[1] % 128 == 0 and own % 8 == 0
    if aligned:
        return fused_device(*arrays)
    return per_device(*arrays)


def solution(mesh):
    placed = (
        P(None, "ep"),
        P("ep"),
        P("ep", "tp"),
        P("ep", "tp"),
        P("ep", "tp"),
        P("ep", "tp"),
        P("tp", "ep"),
        P("ep", "tp", None, None),
        P("ep"),
        P(),
        P("ep", None, "tp"),
        P("ep", None, "tp"),
        P("ep", "tp", None),
        P(),
        P(),
        P("ep", "tp"),
        P("ep", "tp"),
        P("tp", "ep"),
        P("ep"),
    )
    return jax.shard_map(
        any_device,
        mesh=mesh,
        in_specs=placed,
        out_specs=(P(None, "ep"), P("ep", "tp", None, None)),
        check_vma=False,
    )
```

```python
import jax
import jax.numpy as jnp
from jax import lax
from jax.experimental import pallas as pl
from jax.experimental.pallas import tpu as pltpu
from jax.sharding import PartitionSpec as P

D = 2048
KEY_DIM = 128
VAL_DIM = 256


norm_eps = 1e-06
clamp_limit = 7.0
gate_alpha = 1.702


def rotate_half(vectors, positions):
    half_dim = vectors.shape[-1] // 2
    inverse = 1.0 / 10000.0 ** jnp.linspace(0.0, 1.0, half_dim, dtype=jnp.float32)
    angles = positions.astype(jnp.float32)[:, None] * inverse[None, :]
    cosine = jnp.cos(angles)[:, None, :]
    sine_part = jnp.sin(angles)[:, None, :]
    first_half = vectors[..., :half_dim]
    second_half = vectors[..., half_dim:]
    return jnp.concatenate(
        [
            first_half * cosine - second_half * sine_part,
            second_half * cosine + first_half * sine_part,
        ],
        axis=-1,
    )


def slot_index(route_ids, groups, capacity, experts):
    pair_ids = route_ids.reshape(groups, -1)
    labels = jnp.arange(experts, dtype=jnp.int32)
    onehot = (pair_ids[:, :, None] == labels[None, None, :]).astype(jnp.int32)
    earlier = jnp.cumsum(onehot, axis=1) - onehot
    within = jnp.sum(earlier * onehot, axis=2)
    offset = jnp.arange(groups, dtype=jnp.int32)[:, None] * capacity
    return (pair_ids * (groups * capacity) + offset + within).reshape(-1)


def source_rows(target, total_rows, topk_count, table_size):
    owners = jnp.arange(target.shape[0], dtype=jnp.int32) // topk_count
    return jnp.full((table_size,), total_rows, jnp.int32).at[target].set(owners)


def rounded_product(left_rows, right_rows):
    partial_value = jnp.dot(left_rows, right_rows, preferred_element_type=jnp.float32)
    return lax.optimization_barrier(partial_value.astype(jnp.bfloat16))


def per_device(
    residual,
    norm_gain,
    query_weight,
    key_weight,
    value_weight,
    gate_weight,
    out_weight,
    prior_state,
    lengths,
    ffn_gain,
    expert_gate,
    expert_up,
    expert_down,
    route_ids,
    route_weight,
    dense_gate,
    dense_up,
    dense_down,
    mix_vector,
):
    ep_count = lax.axis_size("ep")
    ep_index = lax.axis_index("ep")
    batch_rows, local_width = residual.shape
    own_rows = batch_rows // ep_count
    topk_count = route_ids.shape[1]
    residual_float = residual.astype(jnp.float32)
    squares = jnp.sum(residual_float * residual_float, axis=1)
    normed_in = (residual_float * norm_gain).astype(jnp.bfloat16)
    all_weights = jnp.concatenate([query_weight, key_weight, value_weight, gate_weight], axis=1)
    whole_terms = jnp.dot(normed_in, all_weights, preferred_element_type=jnp.float32)
    projected, own_squares = (
        lax.psum_scatter(whole_terms, "ep", scatter_dimension=0, tiled=True),
        lax.psum_scatter(squares, "ep", scatter_dimension=0, tiled=True),
    )
    row_scale = lax.rsqrt(own_squares / D + norm_eps)[:, None]
    key_cols = query_weight.shape[1]
    value_cols = value_weight.shape[1]
    heads_here = key_cols // KEY_DIM
    projected = projected * row_scale
    query_rot = rotate_half(projected[:, :key_cols].reshape(own_rows, heads_here, KEY_DIM), lengths)
    key_rot = rotate_half(
        projected[:, key_cols : 2 * key_cols].reshape(own_rows, heads_here, KEY_DIM), lengths
    ) * KEY_DIM ** (-0.5)
    values = projected[:, 2 * key_cols : 2 * key_cols + value_cols].reshape(
        own_rows, heads_here, VAL_DIM
    )
    gate_pre = projected[:, 2 * key_cols + value_cols :].reshape(own_rows, heads_here, VAL_DIM)
    head_ids = lax.axis_index("tp") * heads_here + jnp.arange(heads_here, dtype=jnp.int32)
    decay_rate = 1.0 - jnp.exp2(-1.0 - 0.5 * head_ids.astype(jnp.float32))
    new_state = (
        decay_rate[None, :, None, None] * prior_state
        + key_rot[:, :, :, None] * values[:, :, None, :]
    )
    state_read = jnp.einsum("bhk,bhkv->bhv", query_rot, new_state, precision=lax.Precision.HIGHEST)
    normed = state_read * lax.rsqrt(
        jnp.mean(state_read * state_read, axis=-1, keepdims=True) + norm_eps
    )
    gated_out = (
        (normed * jax.nn.silu(gate_pre))
        .astype(jnp.bfloat16)
        .reshape(own_rows, heads_here * VAL_DIM)
    )
    head_terms = rounded_product(lax.all_gather(gated_out, "ep", axis=0, tiled=True), out_weight)
    attn_out = lax.psum(head_terms.astype(jnp.float32).astype(jnp.bfloat16), "tp").astype(
        jnp.float32
    )
    after_mixer = (residual_float + attn_out).astype(jnp.bfloat16)
    capacity = max(2, 2 * own_rows * topk_count // ep_count)
    slot_count = ep_count * capacity
    target = slot_index(route_ids, ep_count, capacity, ep_count)
    slot_source = source_rows(target, batch_rows, topk_count, ep_count * slot_count)
    padded = jnp.concatenate([after_mixer, jnp.zeros((1, local_width), jnp.bfloat16)], axis=0)
    outgoing = padded[slot_source].reshape(ep_count, slot_count, local_width)
    arrived = lax.all_to_all(outgoing, "ep", split_axis=0, concat_axis=2, tiled=True)[0]
    rows_float = arrived.astype(jnp.float32)
    row_norm = lax.rsqrt(jnp.mean(rows_float * rows_float, axis=1, keepdims=True) + norm_eps)
    normed_rows = (rows_float * ffn_gain).astype(jnp.bfloat16)
    gate_val = jnp.minimum(
        jnp.dot(normed_rows, expert_gate[0], preferred_element_type=jnp.float32) * row_norm,
        clamp_limit,
    )
    up_val = jnp.clip(
        jnp.dot(normed_rows, expert_up[0], preferred_element_type=jnp.float32) * row_norm,
        -clamp_limit,
        clamp_limit,
    )
    hidden = ((up_val + 1.0) * gate_val * jax.nn.sigmoid(gate_alpha * gate_val)).astype(
        jnp.bfloat16
    )
    expert_part = rounded_product(hidden, expert_down[0]).astype(jnp.float32)
    expert_sum = lax.psum(expert_part.astype(jnp.bfloat16), "tp")
    returned = lax.all_to_all(expert_sum[None], "ep", split_axis=2, concat_axis=0, tiled=True)
    picked = returned.reshape(ep_count * slot_count, local_width)[target]
    picked = picked.reshape(batch_rows, topk_count, local_width).astype(jnp.float32)
    routed = jnp.sum(picked * route_weight[:, :, None], axis=1)
    after_float = after_mixer.astype(jnp.float32)
    gain_here = lax.dynamic_slice_in_dim(ffn_gain, ep_index * local_width, local_width, 0)
    normed_ffn = (after_float * gain_here).astype(jnp.bfloat16)
    dense_cols = dense_gate.shape[1]
    both_terms = jnp.dot(
        normed_ffn,
        jnp.concatenate([dense_gate, dense_up], axis=1),
        preferred_element_type=jnp.float32,
    )
    mix_term = jnp.dot(normed_ffn, mix_vector, preferred_element_type=jnp.float32)
    both_terms, ffn_squares, mix_logit = lax.psum(
        (both_terms, jnp.sum(after_float * after_float, axis=1), mix_term), "ep"
    )
    ffn_scale = lax.rsqrt(ffn_squares / D + norm_eps)[:, None]
    dense_act = (
        jax.nn.silu(both_terms[:, :dense_cols] * ffn_scale)
        * (both_terms[:, dense_cols:] * ffn_scale)
    ).astype(jnp.bfloat16)
    dense_part = rounded_product(dense_act, dense_down).astype(jnp.float32)
    dense_out = lax.psum(dense_part.astype(jnp.bfloat16), "tp").astype(jnp.float32)
    dense_mix = jax.nn.sigmoid(ffn_scale[:, 0] * mix_logit)
    layer_out = (after_float + routed + dense_mix[:, None] * dense_out).astype(jnp.bfloat16)
    return (layer_out, new_state)


F32 = jnp.float32
BF16 = jnp.bfloat16
MESH = pl.DeviceIdType.MESH
PROJ, SQUARE, MIX, HEAD, ROWS, DENSE_SUM, DENSE_ACT, BACK, QUERY = range(9)
ATTN, FINAL = range(2)


def fused_kernel(
    residual, norm_gain, cosine, sine, gains, route_ids, route_weight, mix_own,
    query_hbm, key_hbm, value_hbm, gate_hbm, out_hbm, prior_hbm,
    egate_hbm, eup_hbm, edown_hbm, dgate_hbm, dup_hbm, ddown_hbm,
    layer_out, key_out, value_out,
    query_w, key_w, value_w, gate_w, out_w, prior, prior_half,
    egate, eup, edown, dgate, dup, ddown,
    query_send, query_recv, proj_send, proj_recv, sq_send, sq_recv, mix_all, heads_all, attn_all,
    rows_all, square_rows, dense_send, dense_recv, act_all, back_send, back_recv, final_all,
    load_sem, send_sem, recv_sem, tp_send, tp_recv,
    relay_send, relay_recv,
):
    _, ep, part_rows, width = rows_all.shape
    batch = 2 * part_rows
    tp = attn_all.shape[0]
    own = batch // ep
    full = ep * width
    me = lax.axis_index("ep")
    lane = lax.axis_index("tp")
    core = lax.rem(lane, 2)
    twin = lane + 1 - 2 * core
    pairs = [
        (query_hbm, query_w), (key_hbm, key_w), (value_hbm, value_w), (gate_hbm, gate_w),
        (prior_hbm, prior), (out_hbm, out_w), (dgate_hbm, dgate), (dup_hbm, dup),
        (egate_hbm, egate), (eup_hbm, eup), (edown_hbm, edown), (ddown_hbm, ddown),
    ]
    loads = [pltpu.make_async_copy(a, b, load_sem.at[i]) for i, (a, b) in enumerate(pairs)]
    barrier = pltpu.get_barrier_semaphore()
    for d in range(1, ep):
        pl.semaphore_signal(
            barrier, inc=1, device_id=(lax.rem(me + d, ep), lane), device_id_type=MESH
        )
    for d in range(1, tp):
        pl.semaphore_signal(
            barrier, inc=1, device_id=(me, lax.rem(lane + d, tp)), device_id_type=MESH
        )
    for load in loads[:4]:
        load.start()

    def to_ep(phase, d, source, target):
        return pltpu.make_async_remote_copy(
            src_ref=source,
            dst_ref=target,
            send_sem=send_sem.at[phase, d],
            recv_sem=recv_sem.at[phase, d],
            device_id=(lax.rem(me + d, ep), lane),
            device_id_type=MESH,
        )

    def to_tp(phase, d, source, target):
        return pltpu.make_async_remote_copy(
            src_ref=source,
            dst_ref=target,
            send_sem=tp_send.at[phase, d],
            recv_sem=tp_recv.at[phase, d],
            device_id=(me, lax.rem(lane + d, tp)),
            device_id_type=MESH,
        )

    sent = []

    def go(copy):
        copy.start()
        sent.append(copy)

    def peer(d):
        return lax.rem(me + d, ep)

    def sender(d):
        return lax.rem(me + ep - d, ep)

    def got(phase, d, buffer):
        to_ep(phase, d, buffer, buffer).wait_recv()

    resid = residual[...].astype(F32)
    squares = jnp.sum(resid * resid, axis=1, keepdims=True)
    squares = jnp.broadcast_to(squares, (batch, sq_send.shape[2]))
    for e in range(ep):
        sq_send[e] = squares[e * own : (e + 1) * own]
    normed_in = (resid * norm_gain[...]).astype(BF16)
    def project(weight, target, offset):
        cols = weight.shape[1]
        step = min(cols, 512)
        for c in range(0, cols, step):
            terms = jnp.dot(normed_in, weight[:, c : c + step], preferred_element_type=F32)
            for e in range(ep):
                target[e, :, offset + c : offset + c + step] = terms[
                    e * own : (e + 1) * own
                ].astype(BF16)

    key_cols = query_w.shape[1]
    value_cols = value_w.shape[1]
    loads[0].wait()
    project(query_w, query_send, 0)
    loads[1].wait()
    project(key_w, proj_send, 0)
    mix_rows = mix_own[...].astype(F32)
    for i in range(width // 128):
        mix_all[me, :, i * 128 : (i + 1) * 128] = mix_rows[i : i + 1]
    pl.semaphore_wait(barrier, ep + tp - 2)
    for d in range(1, ep):
        go(to_ep(SQUARE, d, sq_send.at[peer(d)], sq_recv.at[d]))
        go(to_ep(QUERY, d, query_send.at[peer(d)], query_recv.at[d]))
    loads[2].wait()
    project(value_w, proj_send, key_cols)
    loads[3].wait()
    project(gate_w, proj_send, key_cols + value_cols)
    for d in range(1, ep):
        go(to_ep(PROJ, d, proj_send.at[peer(d)], proj_recv.at[d]))
    for d in range(1, ep):
        go(to_ep(MIX, d, mix_all.at[me], mix_all.at[me]))
    loads[4].start()
    heads = prior.shape[1]
    loads[4].wait()
    for b in range(own):
        for h in range(heads):
            prior_half[b, h] = prior[b, h].astype(BF16)
    for load in loads[5:]:
        load.start()
    route_row = jnp.sum(
        jnp.where(route_ids[...] == me, route_weight[...], 0.0), axis=0, keepdims=True
    )
    diagonal = lax.broadcasted_iota(jnp.int32, (batch, batch), 0) == lax.broadcasted_iota(
        jnp.int32, (batch, batch), 1
    )
    route_col = jnp.sum(jnp.where(diagonal, route_row, 0.0), axis=1, keepdims=True)
    total_sq = sq_send[me]
    queries = query_send[me].astype(F32)
    for d in range(1, ep):
        got(SQUARE, d, sq_recv.at[d])
        total_sq = total_sq + sq_recv[d]
        got(QUERY, d, query_recv.at[d])
        queries = queries + query_recv[d].astype(F32)
    row_scale = lax.rsqrt(total_sq / full + norm_eps)[:, :1]
    queries = queries * row_scale
    row_ids = lax.broadcasted_iota(jnp.int32, (own, VAL_DIM), 0)
    rotated, pasts = [], []
    for h in range(heads):
        q = queries[:, h * KEY_DIM : (h + 1) * KEY_DIM]
        q = q * cosine[...] + pltpu.roll(q, KEY_DIM // 2, 1) * sine[...]
        q_half = q.astype(BF16)
        past = jnp.zeros((own, VAL_DIM), F32)
        for b in range(own):
            every = jnp.dot(q_half, prior_half[b, h], preferred_element_type=F32)
            past = past + jnp.where(row_ids == b, every, 0.0)
        rotated.append(q)
        pasts.append(past)
    projected = proj_send[me].astype(F32)
    for d in range(1, ep):
        got(PROJ, d, proj_recv.at[d])
        projected = projected + proj_recv[d].astype(F32)
    projected = projected * row_scale
    for h in range(heads):
        q, past = rotated[h], pasts[h]
        k = projected[:, h * KEY_DIM : (h + 1) * KEY_DIM]
        k = (k * cosine[...] + pltpu.roll(k, KEY_DIM // 2, 1) * sine[...]) * KEY_DIM ** (-0.5)
        key_out[:, h, :] = k
        start = key_cols + h * VAL_DIM
        v = projected[:, start : start + VAL_DIM]
        value_out[:, h, :] = v
        gate_pre = projected[:, start + value_cols : start + value_cols + VAL_DIM]
        head_id = jnp.full((own, VAL_DIM), lane * heads + h, jnp.int32).astype(F32)
        decay = 1.0 - jnp.exp((head_id * 0.5 + 1.0) * -0.6931471805599453)
        read = decay * past + jnp.sum(q * k, axis=1, keepdims=True) * v
        normed = read * lax.rsqrt(jnp.mean(read * read, axis=1, keepdims=True) + norm_eps)
        heads_all[me, :, h * VAL_DIM : (h + 1) * VAL_DIM] = (
            normed * (gate_pre / (1.0 + jnp.exp(-gate_pre)))
        ).astype(BF16)

    for d in range(1, ep):
        go(to_ep(HEAD, d, heads_all.at[me], heads_all.at[me]))
    loads[5].wait()
    for d in range(1, ep):
        got(HEAD, d, heads_all.at[sender(d)])
    gated = jnp.concatenate([heads_all[e].astype(F32) for e in range(ep)], axis=0)
    attn_all[lane] = jnp.dot(
        gated.astype(BF16), out_w[...], preferred_element_type=F32
    ).astype(BF16)
    for d in range(1, tp):
        go(to_tp(ATTN, d, attn_all.at[lane], attn_all.at[lane]))
    for d in range(1, tp):
        slot = attn_all.at[lax.rem(lane + tp - d, tp)]
        to_tp(ATTN, d, slot, slot).wait_recv()
    attn = attn_all[0].astype(F32)
    for t in range(1, tp):
        attn = attn + attn_all[t].astype(F32)
    after = (resid + attn).astype(BF16)
    rows_all[0, me] = after[:part_rows]
    rows_all[1, me] = after[part_rows:]
    for d in range(1, ep):
        go(to_ep(ROWS, d, rows_all.at[core, me], rows_all.at[core, me]))

    after_float = after.astype(F32)
    own_normed = (after_float * gains[me]).astype(BF16)
    dense_cols = dgate.shape[1]
    for i, weight in enumerate((dgate, dup)):
        loads[6 + i].wait()
        terms = jnp.dot(own_normed, weight[...], preferred_element_type=F32)
        for e in range(ep):
            dense_send[e, :, i * dense_cols : (i + 1) * dense_cols] = terms[
                e * own : (e + 1) * own
            ].astype(BF16)
    for d in range(1, ep):
        go(to_ep(DENSE_SUM, d, dense_send.at[peer(d)], dense_recv.at[d]))

    loads[8].wait()
    loads[9].wait()
    def relay(d, source):
        return pltpu.make_async_remote_copy(
            src_ref=source,
            dst_ref=source,
            send_sem=relay_send.at[d],
            recv_sem=relay_recv.at[d],
            device_id=(me, twin),
            device_id_type=MESH,
        )

    def pass_on(d):
        got(ROWS, d, rows_all.at[core, sender(d)])
        go(relay(d, rows_all.at[core, sender(d)]))

    gate_acc = up_acc = None
    sq_acc = logit = None
    for d in range(ep):
        e = sender(d)
        if d + 1 < ep:
            pass_on(d + 1)
        if d:
            relay(d, rows_all.at[1 - core, e]).wait_recv()
            got(MIX, d, mix_all.at[e])
        z = jnp.concatenate([rows_all[0, e].astype(F32), rows_all[1, e].astype(F32)], axis=0)
        zn = (z * gains[e]).astype(BF16)
        depth = pl.ds(pl.multiple_of(e * width, width), width)
        g = jnp.dot(zn, egate[0, depth, :], preferred_element_type=F32)
        u = jnp.dot(zn, eup[0, depth, :], preferred_element_type=F32)
        s = jnp.sum(z * z, axis=1, keepdims=True)
        m = jnp.sum(zn.astype(F32) * mix_all[e], axis=1, keepdims=True)
        if d:
            gate_acc, up_acc, sq_acc, logit = gate_acc + g, up_acc + u, sq_acc + s, logit + m
        else:
            gate_acc, up_acc, sq_acc, logit = g, u, s, m
    scale = lax.rsqrt(sq_acc / full + norm_eps)
    square_rows[...] = jnp.broadcast_to(scale, square_rows.shape)
    both = dense_send[me].astype(F32)
    for d in range(1, ep):
        got(DENSE_SUM, d, dense_recv.at[d])
        both = both + dense_recv[d].astype(F32)
    both = both * square_rows[pl.ds(pl.multiple_of(me * own, own), own), :][:, :1]
    dg = both[:, :dense_cols]
    act_all[me] = (dg / (1.0 + jnp.exp(-dg)) * both[:, dense_cols:]).astype(BF16)
    for d in range(1, ep):
        go(to_ep(DENSE_ACT, d, act_all.at[me], act_all.at[me]))
    gate_val = jnp.minimum(gate_acc * scale, clamp_limit)
    up_val = jnp.clip(up_acc * scale, -clamp_limit, clamp_limit)
    hidden = ((up_val + 1.0) * gate_val / (1.0 + jnp.exp(-gate_alpha * gate_val))).astype(BF16)
    loads[10].wait()
    for d in list(range(1, ep)) + [0]:
        e = peer(d)
        columns = pl.ds(pl.multiple_of(e * width, width), width)
        part = jnp.dot(hidden, edown[0, :, columns], preferred_element_type=F32) * route_col
        if d:
            back_send[d] = part.astype(BF16)
            go(to_ep(BACK, d, back_send.at[d], back_recv.at[d]))
    mixed = part
    loads[11].wait()
    for d in range(1, ep):
        got(DENSE_ACT, d, act_all.at[sender(d)])
    act = jnp.concatenate([act_all[e].astype(F32) for e in range(ep)], axis=0)
    dense_part = jnp.dot(act.astype(BF16), ddown[...], preferred_element_type=F32)
    mixed = mixed + dense_part / (1.0 + jnp.exp(-(scale * logit)))
    for d in range(1, ep):
        got(BACK, d, back_recv.at[d])
        mixed = mixed + back_recv[d].astype(F32)
    final_all[lane] = mixed.astype(BF16)
    for d in range(1, tp):
        go(to_tp(FINAL, d, final_all.at[lane], final_all.at[lane]))
    for d in range(1, tp):
        slot = final_all.at[lax.rem(lane + tp - d, tp)]
        to_tp(FINAL, d, slot, slot).wait_recv()
    result = after_float
    for t in range(tp):
        result = result + final_all[t].astype(F32)
    layer_out[...] = result.astype(BF16)
    for copy in sent:
        copy.wait_send()


def fused_device(
    residual, norm_gain, query_weight, key_weight, value_weight, gate_weight, out_weight,
    prior_state, lengths, ffn_gain, expert_gate, expert_up, expert_down, route_ids,
    route_weight, dense_gate, dense_up, dense_down, mix_vector,
):
    ep, tp = lax.axis_size("ep"), lax.axis_size("tp")
    batch, width = residual.shape
    own, heads = prior_state.shape[:2]
    half = KEY_DIM // 2
    inverse = 1.0 / 10000.0 ** jnp.linspace(0.0, 1.0, half, dtype=F32)
    angles = lengths.astype(F32)[:, None] * inverse[None, :]
    cosine, sine = jnp.cos(angles), jnp.sin(angles)
    cosine = jnp.concatenate([cosine, cosine], axis=1)
    sine = jnp.concatenate([-sine, sine], axis=1)
    key_cols, value_cols = query_weight.shape[1], value_weight.shape[1]
    all_cols = key_cols + 2 * value_cols
    dense_cols = dense_gate.shape[1]
    large = (
        query_weight, key_weight, value_weight, gate_weight, out_weight, prior_state,
        expert_gate, expert_up, expert_down, dense_gate, dense_up, dense_down,
    )
    held = [pltpu.VMEM(a.shape, a.dtype) for a in large]
    held.insert(6, pltpu.VMEM(prior_state.shape, BF16))
    vmem = pl.BlockSpec(memory_space=pltpu.VMEM)
    scratch = held + [
        pltpu.VMEM((ep, own, key_cols), BF16),
        pltpu.VMEM((ep, own, key_cols), BF16),
        pltpu.VMEM((ep, own, all_cols), BF16),
        pltpu.VMEM((ep, own, all_cols), BF16),
        pltpu.VMEM((ep, own, 128), F32),
        pltpu.VMEM((ep, own, 128), F32),
        pltpu.VMEM((ep, 1, width), F32),
        pltpu.VMEM((ep, own, value_cols), BF16),
        pltpu.VMEM((tp, batch, width), BF16),
        pltpu.VMEM((2, ep, batch // 2, width), BF16),
        pltpu.VMEM((batch, 128), F32),
        pltpu.VMEM((ep, own, 2 * dense_cols), BF16),
        pltpu.VMEM((ep, own, 2 * dense_cols), BF16),
        pltpu.VMEM((ep, own, dense_cols), BF16),
        pltpu.VMEM((ep, batch, width), BF16),
        pltpu.VMEM((ep, batch, width), BF16),
        pltpu.VMEM((tp, batch, width), BF16),
        pltpu.SemaphoreType.DMA((12,)),
        pltpu.SemaphoreType.DMA((9, ep)),
        pltpu.SemaphoreType.DMA((9, ep)),
        pltpu.SemaphoreType.DMA((2, tp)),
        pltpu.SemaphoreType.DMA((2, tp)),
        pltpu.SemaphoreType.DMA((ep,)),
        pltpu.SemaphoreType.DMA((ep,)),
    ]
    layer_out, key_rot, values = pl.pallas_call(
        fused_kernel,
        out_shape=(
            jax.ShapeDtypeStruct((batch, width), BF16),
            jax.ShapeDtypeStruct((own, heads, KEY_DIM), F32),
            jax.ShapeDtypeStruct((own, heads, VAL_DIM), F32),
        ),
        in_specs=[vmem] * 8 + [pl.BlockSpec(memory_space=pl.ANY)] * 12,
        out_specs=(vmem, vmem, vmem),
        scratch_shapes=scratch,
        compiler_params=pltpu.CompilerParams(
            collective_id=0, has_side_effects=True, vmem_limit_bytes=56 * 1024 * 1024
        ),
    )(
        residual, norm_gain[None, :], cosine, sine, ffn_gain.reshape(ep, 1, width),
        route_ids.T, route_weight.T, mix_vector.reshape(-1, 128), *large,
    )
    head_ids = lax.axis_index("tp") * heads + jnp.arange(heads, dtype=jnp.int32)
    decay_rate = 1.0 - jnp.exp2(-1.0 - 0.5 * head_ids.astype(F32))
    new_state = (
        decay_rate[None, :, None, None] * prior_state
        + key_rot[:, :, :, None] * values[:, :, None, :]
    )
    return (layer_out, new_state)


def any_device(*arrays):
    residual, prior_state, dense_gate = arrays[0], arrays[7], arrays[15]
    own = prior_state.shape[0]
    even = lax.axis_size("tp") % 2 == 0 and residual.shape[0] % 32 == 0
    aligned = even and residual.shape[1] % 128 == 0 and dense_gate.shape[1] % 128 == 0 and own % 8 == 0
    if aligned:
        return fused_device(*arrays)
    return per_device(*arrays)


def solution(mesh):
    placed = (
        P(None, "ep"),
        P("ep"),
        P("ep", "tp"),
        P("ep", "tp"),
        P("ep", "tp"),
        P("ep", "tp"),
        P("tp", "ep"),
        P("ep", "tp", None, None),
        P("ep"),
        P(),
        P("ep", None, "tp"),
        P("ep", None, "tp"),
        P("ep", "tp", None),
        P(),
        P(),
        P("ep", "tp"),
        P("ep", "tp"),
        P("tp", "ep"),
        P("ep"),
    )
    return jax.shard_map(
        any_device,
        mesh=mesh,
        in_specs=placed,
        out_specs=(P(None, "ep"), P("ep", "tp", None, None)),
        check_vma=False,
    )
```

```python
import jax
import jax.numpy as jnp
from jax import lax
from jax.experimental import pallas as pl
from jax.experimental.pallas import tpu as pltpu
from jax.sharding import PartitionSpec as P

D = 2048
KEY_DIM = 128
VAL_DIM = 256


norm_eps = 1e-06
clamp_limit = 7.0
gate_alpha = 1.702


def rotate_half(vectors, positions):
    half_dim = vectors.shape[-1] // 2
    inverse = 1.0 / 10000.0 ** jnp.linspace(0.0, 1.0, half_dim, dtype=jnp.float32)
    angles = positions.astype(jnp.float32)[:, None] * inverse[None, :]
    cosine = jnp.cos(angles)[:, None, :]
    sine_part = jnp.sin(angles)[:, None, :]
    first_half = vectors[..., :half_dim]
    second_half = vectors[..., half_dim:]
    return jnp.concatenate(
        [
            first_half * cosine - second_half * sine_part,
            second_half * cosine + first_half * sine_part,
        ],
        axis=-1,
    )


def slot_index(route_ids, groups, capacity, experts):
    pair_ids = route_ids.reshape(groups, -1)
    labels = jnp.arange(experts, dtype=jnp.int32)
    onehot = (pair_ids[:, :, None] == labels[None, None, :]).astype(jnp.int32)
    earlier = jnp.cumsum(onehot, axis=1) - onehot
    within = jnp.sum(earlier * onehot, axis=2)
    offset = jnp.arange(groups, dtype=jnp.int32)[:, None] * capacity
    return (pair_ids * (groups * capacity) + offset + within).reshape(-1)


def source_rows(target, total_rows, topk_count, table_size):
    owners = jnp.arange(target.shape[0], dtype=jnp.int32) // topk_count
    return jnp.full((table_size,), total_rows, jnp.int32).at[target].set(owners)


def rounded_product(left_rows, right_rows):
    partial_value = jnp.dot(left_rows, right_rows, preferred_element_type=jnp.float32)
    return lax.optimization_barrier(partial_value.astype(jnp.bfloat16))


def per_device(
    residual,
    norm_gain,
    query_weight,
    key_weight,
    value_weight,
    gate_weight,
    out_weight,
    prior_state,
    lengths,
    ffn_gain,
    expert_gate,
    expert_up,
    expert_down,
    route_ids,
    route_weight,
    dense_gate,
    dense_up,
    dense_down,
    mix_vector,
):
    ep_count = lax.axis_size("ep")
    ep_index = lax.axis_index("ep")
    batch_rows, local_width = residual.shape
    own_rows = batch_rows // ep_count
    topk_count = route_ids.shape[1]
    residual_float = residual.astype(jnp.float32)
    squares = jnp.sum(residual_float * residual_float, axis=1)
    normed_in = (residual_float * norm_gain).astype(jnp.bfloat16)
    all_weights = jnp.concatenate([query_weight, key_weight, value_weight, gate_weight], axis=1)
    whole_terms = jnp.dot(normed_in, all_weights, preferred_element_type=jnp.float32)
    projected, own_squares = (
        lax.psum_scatter(whole_terms, "ep", scatter_dimension=0, tiled=True),
        lax.psum_scatter(squares, "ep", scatter_dimension=0, tiled=True),
    )
    row_scale = lax.rsqrt(own_squares / D + norm_eps)[:, None]
    key_cols = query_weight.shape[1]
    value_cols = value_weight.shape[1]
    heads_here = key_cols // KEY_DIM
    projected = projected * row_scale
    query_rot = rotate_half(projected[:, :key_cols].reshape(own_rows, heads_here, KEY_DIM), lengths)
    key_rot = rotate_half(
        projected[:, key_cols : 2 * key_cols].reshape(own_rows, heads_here, KEY_DIM), lengths
    ) * KEY_DIM ** (-0.5)
    values = projected[:, 2 * key_cols : 2 * key_cols + value_cols].reshape(
        own_rows, heads_here, VAL_DIM
    )
    gate_pre = projected[:, 2 * key_cols + value_cols :].reshape(own_rows, heads_here, VAL_DIM)
    head_ids = lax.axis_index("tp") * heads_here + jnp.arange(heads_here, dtype=jnp.int32)
    decay_rate = 1.0 - jnp.exp2(-1.0 - 0.5 * head_ids.astype(jnp.float32))
    new_state = (
        decay_rate[None, :, None, None] * prior_state
        + key_rot[:, :, :, None] * values[:, :, None, :]
    )
    state_read = jnp.einsum("bhk,bhkv->bhv", query_rot, new_state, precision=lax.Precision.HIGHEST)
    normed = state_read * lax.rsqrt(
        jnp.mean(state_read * state_read, axis=-1, keepdims=True) + norm_eps
    )
    gated_out = (
        (normed * jax.nn.silu(gate_pre))
        .astype(jnp.bfloat16)
        .reshape(own_rows, heads_here * VAL_DIM)
    )
    head_terms = rounded_product(lax.all_gather(gated_out, "ep", axis=0, tiled=True), out_weight)
    attn_out = lax.psum(head_terms.astype(jnp.float32).astype(jnp.bfloat16), "tp").astype(
        jnp.float32
    )
    after_mixer = (residual_float + attn_out).astype(jnp.bfloat16)
    capacity = max(2, 2 * own_rows * topk_count // ep_count)
    slot_count = ep_count * capacity
    target = slot_index(route_ids, ep_count, capacity, ep_count)
    slot_source = source_rows(target, batch_rows, topk_count, ep_count * slot_count)
    padded = jnp.concatenate([after_mixer, jnp.zeros((1, local_width), jnp.bfloat16)], axis=0)
    outgoing = padded[slot_source].reshape(ep_count, slot_count, local_width)
    arrived = lax.all_to_all(outgoing, "ep", split_axis=0, concat_axis=2, tiled=True)[0]
    rows_float = arrived.astype(jnp.float32)
    row_norm = lax.rsqrt(jnp.mean(rows_float * rows_float, axis=1, keepdims=True) + norm_eps)
    normed_rows = (rows_float * ffn_gain).astype(jnp.bfloat16)
    gate_val = jnp.minimum(
        jnp.dot(normed_rows, expert_gate[0], preferred_element_type=jnp.float32) * row_norm,
        clamp_limit,
    )
    up_val = jnp.clip(
        jnp.dot(normed_rows, expert_up[0], preferred_element_type=jnp.float32) * row_norm,
        -clamp_limit,
        clamp_limit,
    )
    hidden = ((up_val + 1.0) * gate_val * jax.nn.sigmoid(gate_alpha * gate_val)).astype(
        jnp.bfloat16
    )
    expert_part = rounded_product(hidden, expert_down[0]).astype(jnp.float32)
    expert_sum = lax.psum(expert_part.astype(jnp.bfloat16), "tp")
    returned = lax.all_to_all(expert_sum[None], "ep", split_axis=2, concat_axis=0, tiled=True)
    picked = returned.reshape(ep_count * slot_count, local_width)[target]
    picked = picked.reshape(batch_rows, topk_count, local_width).astype(jnp.float32)
    routed = jnp.sum(picked * route_weight[:, :, None], axis=1)
    after_float = after_mixer.astype(jnp.float32)
    gain_here = lax.dynamic_slice_in_dim(ffn_gain, ep_index * local_width, local_width, 0)
    normed_ffn = (after_float * gain_here).astype(jnp.bfloat16)
    dense_cols = dense_gate.shape[1]
    both_terms = jnp.dot(
        normed_ffn,
        jnp.concatenate([dense_gate, dense_up], axis=1),
        preferred_element_type=jnp.float32,
    )
    mix_term = jnp.dot(normed_ffn, mix_vector, preferred_element_type=jnp.float32)
    both_terms, ffn_squares, mix_logit = lax.psum(
        (both_terms, jnp.sum(after_float * after_float, axis=1), mix_term), "ep"
    )
    ffn_scale = lax.rsqrt(ffn_squares / D + norm_eps)[:, None]
    dense_act = (
        jax.nn.silu(both_terms[:, :dense_cols] * ffn_scale)
        * (both_terms[:, dense_cols:] * ffn_scale)
    ).astype(jnp.bfloat16)
    dense_part = rounded_product(dense_act, dense_down).astype(jnp.float32)
    dense_out = lax.psum(dense_part.astype(jnp.bfloat16), "tp").astype(jnp.float32)
    dense_mix = jax.nn.sigmoid(ffn_scale[:, 0] * mix_logit)
    layer_out = (after_float + routed + dense_mix[:, None] * dense_out).astype(jnp.bfloat16)
    return (layer_out, new_state)


F32 = jnp.float32
BF16 = jnp.bfloat16
MESH = pl.DeviceIdType.MESH
PROJ, SQUARE, MIX, HEAD, ROWS, DENSE_SUM, DENSE_ACT, BACK, QUERY = range(9)
ATTN, FINAL = range(2)


def fused_kernel(
    residual, norm_gain, cosine, sine, gains, route_ids, route_weight, mix_own,
    query_hbm, key_hbm, value_hbm, gate_hbm, out_hbm, prior_hbm,
    egate_hbm, eup_hbm, edown_hbm, dgate_hbm, dup_hbm, ddown_hbm,
    layer_out, key_out, value_out,
    query_w, key_w, value_w, gate_w, out_w, prior, prior_half,
    egate, eup, edown, dgate, dup, ddown,
    query_send, query_recv, proj_send, proj_recv, sq_send, sq_recv, mix_all, heads_all, attn_all,
    rows_all, square_rows, dense_send, dense_recv, act_all, back_send, back_recv, final_all,
    load_sem, send_sem, recv_sem, tp_send, tp_recv,
    relay_send, relay_recv, twin_out, twin_in, kept, halves, twin_send, twin_recv,
):
    _, ep, part_rows, width = rows_all.shape
    batch = 2 * part_rows
    tp = attn_all.shape[0]
    own = batch // ep
    full = ep * width
    me = lax.axis_index("ep")
    lane = lax.axis_index("tp")
    core = lax.rem(lane, 2)
    twin = lane + 1 - 2 * core
    pairs = [
        (query_hbm, query_w), (key_hbm, key_w), (value_hbm, value_w), (gate_hbm, gate_w),
        (prior_hbm, prior), (out_hbm, out_w), (dgate_hbm, dgate), (dup_hbm, dup),
        (egate_hbm, egate), (eup_hbm, eup), (edown_hbm, edown), (ddown_hbm, ddown),
    ]
    loads = [pltpu.make_async_copy(a, b, load_sem.at[i]) for i, (a, b) in enumerate(pairs)]
    barrier = pltpu.get_barrier_semaphore()
    for d in range(1, ep):
        pl.semaphore_signal(
            barrier, inc=1, device_id=(lax.rem(me + d, ep), lane), device_id_type=MESH
        )
    for d in range(1, tp):
        pl.semaphore_signal(
            barrier, inc=1, device_id=(me, lax.rem(lane + d, tp)), device_id_type=MESH
        )
    for load in loads[:4]:
        load.start()

    def to_ep(phase, d, source, target):
        return pltpu.make_async_remote_copy(
            src_ref=source,
            dst_ref=target,
            send_sem=send_sem.at[phase, d],
            recv_sem=recv_sem.at[phase, d],
            device_id=(lax.rem(me + d, ep), lane),
            device_id_type=MESH,
        )

    def to_tp(phase, d, source, target):
        return pltpu.make_async_remote_copy(
            src_ref=source,
            dst_ref=target,
            send_sem=tp_send.at[phase, d],
            recv_sem=tp_recv.at[phase, d],
            device_id=(me, lax.rem(lane + d, tp)),
            device_id_type=MESH,
        )

    sent = []

    def go(copy):
        copy.start()
        sent.append(copy)

    def peer(d):
        return lax.rem(me + d, ep)

    def sender(d):
        return lax.rem(me + ep - d, ep)

    def got(phase, d, buffer):
        to_ep(phase, d, buffer, buffer).wait_recv()

    resid = residual[...].astype(F32)
    squares = jnp.sum(resid * resid, axis=1, keepdims=True)
    squares = jnp.broadcast_to(squares, (batch, sq_send.shape[2]))
    for e in range(ep):
        sq_send[e] = squares[e * own : (e + 1) * own]
    normed_in = (resid * norm_gain[...]).astype(BF16)
    def project(weight, target, offset):
        cols = weight.shape[1]
        step = min(cols, 512)
        for c in range(0, cols, step):
            terms = jnp.dot(normed_in, weight[:, c : c + step], preferred_element_type=F32)
            for e in range(ep):
                target[e, :, offset + c : offset + c + step] = terms[
                    e * own : (e + 1) * own
                ].astype(BF16)

    key_cols = query_w.shape[1]
    value_cols = value_w.shape[1]
    loads[0].wait()
    project(query_w, query_send, 0)
    loads[1].wait()
    project(key_w, proj_send, 0)
    mix_rows = mix_own[...].astype(F32)
    for i in range(width // 128):
        mix_all[me, :, i * 128 : (i + 1) * 128] = mix_rows[i : i + 1]
    pl.semaphore_wait(barrier, ep + tp - 2)
    for d in range(1, ep):
        go(to_ep(SQUARE, d, sq_send.at[peer(d)], sq_recv.at[d]))
        go(to_ep(QUERY, d, query_send.at[peer(d)], query_recv.at[d]))
    loads[2].wait()
    project(value_w, proj_send, key_cols)
    loads[3].wait()
    project(gate_w, proj_send, key_cols + value_cols)
    for d in range(1, ep):
        go(to_ep(PROJ, d, proj_send.at[peer(d)], proj_recv.at[d]))
    for d in range(1, ep):
        go(to_ep(MIX, d, mix_all.at[me], mix_all.at[me]))
    loads[4].start()
    heads = prior.shape[1]
    loads[4].wait()
    for b in range(own):
        for h in range(heads):
            prior_half[b, h] = prior[b, h].astype(BF16)
    for load in loads[5:]:
        load.start()
    route_row = jnp.sum(
        jnp.where(route_ids[...] == me, route_weight[...], 0.0), axis=0, keepdims=True
    )
    diagonal = lax.broadcasted_iota(jnp.int32, (batch, batch), 0) == lax.broadcasted_iota(
        jnp.int32, (batch, batch), 1
    )
    route_col = jnp.sum(jnp.where(diagonal, route_row, 0.0), axis=1, keepdims=True)
    total_sq = sq_send[me]
    queries = query_send[me].astype(F32)
    for d in range(1, ep):
        got(SQUARE, d, sq_recv.at[d])
        total_sq = total_sq + sq_recv[d]
        got(QUERY, d, query_recv.at[d])
        queries = queries + query_recv[d].astype(F32)
    row_scale = lax.rsqrt(total_sq / full + norm_eps)[:, :1]
    queries = queries * row_scale
    row_ids = lax.broadcasted_iota(jnp.int32, (own, VAL_DIM), 0)
    rotated, pasts = [], []
    turn_cos = jnp.concatenate([cosine[...], cosine[...]], axis=1)
    turn_sin = jnp.concatenate([-sine[...], sine[...]], axis=1)
    for h in range(heads):
        q = queries[:, h * KEY_DIM : (h + 1) * KEY_DIM]
        q = q * turn_cos + pltpu.roll(q, KEY_DIM // 2, 1) * turn_sin
        q_half = q.astype(BF16)
        past = jnp.zeros((own, VAL_DIM), F32)
        for b in range(own):
            every = jnp.dot(q_half, prior_half[b, h], preferred_element_type=F32)
            past = past + jnp.where(row_ids == b, every, 0.0)
        rotated.append(q)
        pasts.append(past)
    projected = proj_send[me].astype(F32)
    for d in range(1, ep):
        got(PROJ, d, proj_recv.at[d])
        projected = projected + proj_recv[d].astype(F32)
    projected = projected * row_scale
    for h in range(heads):
        q, past = rotated[h], pasts[h]
        k = projected[:, h * KEY_DIM : (h + 1) * KEY_DIM]
        k = (k * turn_cos + pltpu.roll(k, KEY_DIM // 2, 1) * turn_sin) * KEY_DIM ** (-0.5)
        key_out[:, h, :] = k
        start = key_cols + h * VAL_DIM
        v = projected[:, start : start + VAL_DIM]
        value_out[:, h, :] = v
        gate_pre = projected[:, start + value_cols : start + value_cols + VAL_DIM]
        head_id = jnp.full((own, VAL_DIM), lane * heads + h, jnp.int32).astype(F32)
        decay = 1.0 - jnp.exp((head_id * 0.5 + 1.0) * -0.6931471805599453)
        read = decay * past + jnp.sum(q * k, axis=1, keepdims=True) * v
        normed = read * lax.rsqrt(jnp.mean(read * read, axis=1, keepdims=True) + norm_eps)
        heads_all[me, :, h * VAL_DIM : (h + 1) * VAL_DIM] = (
            normed * (gate_pre / (1.0 + jnp.exp(-gate_pre)))
        ).astype(BF16)

    for d in range(1, ep):
        go(to_ep(HEAD, d, heads_all.at[me], heads_all.at[me]))
    loads[5].wait()
    for d in range(1, ep):
        got(HEAD, d, heads_all.at[sender(d)])
    gated = jnp.concatenate([heads_all[e].astype(F32) for e in range(ep)], axis=0)
    attn_all[lane] = jnp.dot(
        gated.astype(BF16), out_w[...], preferred_element_type=F32
    ).astype(BF16)
    for d in range(1, tp):
        go(to_tp(ATTN, d, attn_all.at[lane], attn_all.at[lane]))
    for d in range(1, tp):
        slot = attn_all.at[lax.rem(lane + tp - d, tp)]
        to_tp(ATTN, d, slot, slot).wait_recv()
    attn = attn_all[0].astype(F32)
    for t in range(1, tp):
        attn = attn + attn_all[t].astype(F32)
    after = (resid + attn).astype(BF16)
    rows_all[0, me] = after[:part_rows]
    rows_all[1, me] = after[part_rows:]
    for d in range(1, ep):
        go(to_ep(ROWS, d, rows_all.at[core, me], rows_all.at[core, me]))

    after_float = after.astype(F32)
    own_normed = (after_float * gains[me]).astype(BF16)
    dense_cols = dgate.shape[1]
    for i, weight in enumerate((dgate, dup)):
        loads[6 + i].wait()
        terms = jnp.dot(own_normed, weight[...], preferred_element_type=F32)
        for e in range(ep):
            dense_send[e, :, i * dense_cols : (i + 1) * dense_cols] = terms[
                e * own : (e + 1) * own
            ].astype(BF16)
    for d in range(1, ep):
        go(to_ep(DENSE_SUM, d, dense_send.at[peer(d)], dense_recv.at[d]))

    loads[8].wait()
    loads[9].wait()
    def relay(d, source):
        return pltpu.make_async_remote_copy(
            src_ref=source,
            dst_ref=source,
            send_sem=relay_send.at[d],
            recv_sem=relay_recv.at[d],
            device_id=(me, twin),
            device_id_type=MESH,
        )

    def pass_on(d):
        got(ROWS, d, rows_all.at[core, sender(d)])
        go(relay(d, rows_all.at[core, sender(d)]))

    gate_acc = up_acc = None
    sq_acc = logit = None
    for d in range(ep):
        e = sender(d)
        if d + 1 < ep:
            pass_on(d + 1)
        if d:
            relay(d, rows_all.at[1 - core, e]).wait_recv()
            got(MIX, d, mix_all.at[e])
        z = jnp.concatenate([rows_all[0, e].astype(F32), rows_all[1, e].astype(F32)], axis=0)
        zn = (z * gains[e]).astype(BF16)
        depth = pl.ds(pl.multiple_of(e * width, width), width)
        g = jnp.dot(zn, egate[0, depth, :], preferred_element_type=F32)
        u = jnp.dot(zn, eup[0, depth, :], preferred_element_type=F32)
        s = jnp.sum(z * z, axis=1, keepdims=True)
        m = jnp.sum(zn.astype(F32) * mix_all[e], axis=1, keepdims=True)
        if d:
            gate_acc, up_acc, sq_acc, logit = gate_acc + g, up_acc + u, sq_acc + s, logit + m
        else:
            gate_acc, up_acc, sq_acc, logit = g, u, s, m
    scale = lax.rsqrt(sq_acc / full + norm_eps)
    square_rows[...] = jnp.broadcast_to(scale, square_rows.shape)
    both = dense_send[me].astype(F32)
    for d in range(1, ep):
        got(DENSE_SUM, d, dense_recv.at[d])
        both = both + dense_recv[d].astype(F32)
    both = both * square_rows[pl.ds(pl.multiple_of(me * own, own), own), :][:, :1]
    dg = both[:, :dense_cols]
    act_all[me] = (dg / (1.0 + jnp.exp(-dg)) * both[:, dense_cols:]).astype(BF16)
    for d in range(1, ep):
        go(to_ep(DENSE_ACT, d, act_all.at[me], act_all.at[me]))
    gate_val = jnp.minimum(gate_acc * scale, clamp_limit)
    up_val = jnp.clip(up_acc * scale, -clamp_limit, clamp_limit)
    hidden = ((up_val + 1.0) * gate_val / (1.0 + jnp.exp(-gate_alpha * gate_val))).astype(BF16)
    loads[10].wait()
    first = jnp.full((part_rows, width), core, jnp.int32) == 0

    def split(whole):
        low, high = whole[:part_rows], whole[part_rows:]
        return jnp.where(first, low, high), jnp.where(first, high, low)

    def to_twin(i, source, target):
        return pltpu.make_async_remote_copy(
            src_ref=source,
            dst_ref=target,
            send_sem=twin_send.at[i],
            recv_sem=twin_recv.at[i],
            device_id=(me, twin),
            device_id_type=MESH,
        )

    def hand_over(i, whole):
        mine, other = split(whole)
        kept[i] = mine
        twin_out[i] = other.astype(BF16)
        go(to_twin(i, twin_out.at[i], twin_in.at[i]))

    def joined(i):
        to_twin(i, twin_in.at[i], twin_in.at[i]).wait_recv()
        return kept[i] + twin_in[i].astype(F32)

    def give_back(d):
        back_send[d] = joined(d).astype(BF16)
        go(to_ep(BACK, d, back_send.at[d], back_recv.at[d]))

    turns = list(range(1, ep)) + [0]
    lag = min(3, ep - 1)
    for i, d in enumerate(turns):
        columns = pl.ds(pl.multiple_of(peer(d) * width, width), width)
        part = jnp.dot(hidden, edown[0, :, columns], preferred_element_type=F32) * route_col
        hand_over(d, part)
        if i >= lag:
            give_back(turns[i - lag])
    for d in turns[ep - lag : ep - 1]:
        give_back(d)
    loads[11].wait()
    for d in range(1, ep):
        got(DENSE_ACT, d, act_all.at[sender(d)])
    act = jnp.concatenate([act_all[e].astype(F32) for e in range(ep)], axis=0)
    dense_part = jnp.dot(act.astype(BF16), ddown[...], preferred_element_type=F32)
    hand_over(ep, dense_part / (1.0 + jnp.exp(-(scale * logit))))
    mixed = joined(0) + joined(ep)
    for d in range(1, ep):
        got(BACK, d, back_recv.at[d])
        mixed = mixed + back_recv[d].astype(F32)
    final_all[lane] = mixed.astype(BF16)
    for d in range(2, tp, 2):
        go(to_tp(FINAL, d, final_all.at[lane], final_all.at[lane]))
    for d in range(2, tp, 2):
        slot = final_all.at[lax.rem(lane + tp - d, tp)]
        to_tp(FINAL, d, slot, slot).wait_recv()
    result, _ = split(after_float)
    for t in range(tp // 2):
        result = result + final_all[core + 2 * t].astype(F32)
    halves[core] = result.astype(BF16)
    go(to_twin(ep + 1, halves.at[core], halves.at[core]))
    to_twin(ep + 1, halves.at[1 - core], halves.at[1 - core]).wait_recv()
    layer_out[:part_rows] = halves[0]
    layer_out[part_rows:] = halves[1]
    for copy in sent:
        copy.wait_send()


def fused_device(
    residual, norm_gain, query_weight, key_weight, value_weight, gate_weight, out_weight,
    prior_state, lengths, ffn_gain, expert_gate, expert_up, expert_down, route_ids,
    route_weight, dense_gate, dense_up, dense_down, mix_vector,
):
    ep, tp = lax.axis_size("ep"), lax.axis_size("tp")
    batch, width = residual.shape
    own, heads = prior_state.shape[:2]
    half = KEY_DIM // 2
    inverse = 1.0 / 10000.0 ** jnp.linspace(0.0, 1.0, half, dtype=F32)
    angles = lengths.astype(F32)[:, None] * inverse[None, :]
    cosine, sine = jnp.cos(angles), jnp.sin(angles)
    key_cols, value_cols = query_weight.shape[1], value_weight.shape[1]
    all_cols = key_cols + 2 * value_cols
    dense_cols = dense_gate.shape[1]
    large = (
        query_weight, key_weight, value_weight, gate_weight, out_weight, prior_state,
        expert_gate, expert_up, expert_down, dense_gate, dense_up, dense_down,
    )
    held = [pltpu.VMEM(a.shape, a.dtype) for a in large]
    held.insert(6, pltpu.VMEM(prior_state.shape, BF16))
    vmem = pl.BlockSpec(memory_space=pltpu.VMEM)
    scratch = held + [
        pltpu.VMEM((ep, own, key_cols), BF16),
        pltpu.VMEM((ep, own, key_cols), BF16),
        pltpu.VMEM((ep, own, all_cols), BF16),
        pltpu.VMEM((ep, own, all_cols), BF16),
        pltpu.VMEM((ep, own, 128), F32),
        pltpu.VMEM((ep, own, 128), F32),
        pltpu.VMEM((ep, 1, width), F32),
        pltpu.VMEM((ep, own, value_cols), BF16),
        pltpu.VMEM((tp, batch, width), BF16),
        pltpu.VMEM((2, ep, batch // 2, width), BF16),
        pltpu.VMEM((batch, 128), F32),
        pltpu.VMEM((ep, own, 2 * dense_cols), BF16),
        pltpu.VMEM((ep, own, 2 * dense_cols), BF16),
        pltpu.VMEM((ep, own, dense_cols), BF16),
        pltpu.VMEM((ep, batch // 2, width), BF16),
        pltpu.VMEM((ep, batch // 2, width), BF16),
        pltpu.VMEM((tp, batch // 2, width), BF16),
        pltpu.SemaphoreType.DMA((12,)),
        pltpu.SemaphoreType.DMA((9, ep)),
        pltpu.SemaphoreType.DMA((9, ep)),
        pltpu.SemaphoreType.DMA((2, tp)),
        pltpu.SemaphoreType.DMA((2, tp)),
        pltpu.SemaphoreType.DMA((ep,)),
        pltpu.SemaphoreType.DMA((ep,)),
        pltpu.VMEM((ep + 1, batch // 2, width), BF16),
        pltpu.VMEM((ep + 1, batch // 2, width), BF16),
        pltpu.VMEM((ep + 1, batch // 2, width), F32),
        pltpu.VMEM((2, batch // 2, width), BF16),
        pltpu.SemaphoreType.DMA((ep + 2,)),
        pltpu.SemaphoreType.DMA((ep + 2,)),
    ]
    layer_out, key_rot, values = pl.pallas_call(
        fused_kernel,
        out_shape=(
            jax.ShapeDtypeStruct((batch, width), BF16),
            jax.ShapeDtypeStruct((own, heads, KEY_DIM), F32),
            jax.ShapeDtypeStruct((own, heads, VAL_DIM), F32),
        ),
        in_specs=[vmem] * 8 + [pl.BlockSpec(memory_space=pl.ANY)] * 12,
        out_specs=(vmem, vmem, vmem),
        scratch_shapes=scratch,
        compiler_params=pltpu.CompilerParams(
            collective_id=0, has_side_effects=True, vmem_limit_bytes=56 * 1024 * 1024
        ),
    )(
        residual, norm_gain[None, :], cosine, sine, ffn_gain.reshape(ep, 1, width),
        route_ids.T, route_weight.T, mix_vector.reshape(-1, 128), *large,
    )
    head_ids = lax.axis_index("tp") * heads + jnp.arange(heads, dtype=jnp.int32)
    decay_rate = 1.0 - jnp.exp2(-1.0 - 0.5 * head_ids.astype(F32))
    new_state = (
        decay_rate[None, :, None, None] * prior_state
        + key_rot[:, :, :, None] * values[:, :, None, :]
    )
    return (layer_out, new_state)


def any_device(*arrays):
    residual, prior_state, dense_gate = arrays[0], arrays[7], arrays[15]
    own = prior_state.shape[0]
    even = lax.axis_size("tp") % 2 == 0 and residual.shape[0] % 32 == 0
    aligned = even and residual.shape[1] % 128 == 0 and dense_gate.shape[1] % 128 == 0 and own % 8 == 0
    if aligned:
        return fused_device(*arrays)
    return per_device(*arrays)


def solution(mesh):
    placed = (
        P(None, "ep"),
        P("ep"),
        P("ep", "tp"),
        P("ep", "tp"),
        P("ep", "tp"),
        P("ep", "tp"),
        P("tp", "ep"),
        P("ep", "tp", None, None),
        P("ep"),
        P(),
        P("ep", None, "tp"),
        P("ep", None, "tp"),
        P("ep", "tp", None),
        P(),
        P(),
        P("ep", "tp"),
        P("ep", "tp"),
        P("tp", "ep"),
        P("ep"),
    )
    return jax.shard_map(
        any_device,
        mesh=mesh,
        in_specs=placed,
        out_specs=(P(None, "ep"), P("ep", "tp", None, None)),
        check_vma=False,
    )
```
